512 devices in a mesh: sp: 128 (over z, y, core), tp: 4 (over x).
Axes of the slice: x: 4, y: 8, z: 8, core: 2. Of those that a mesh axis runs over, the one named last changes fastest.
Arguments:
- tokens: bfloat16 [32768, 2048], P(('sp', 'tp')), may hold values from -16 to 16
- w_query: bfloat16 [2048, 1024], P(None, 'tp'), may hold values from -1 to 1
- w_key: bfloat16 [2048, 256], P(None, 'tp'), may hold values from -1 to 1
- w_value: bfloat16 [2048, 256], P(None, 'tp'), may hold values from -0.125 to 0.125
- w_gate: bfloat16 [2048, 16], P(None, 'tp'), may hold values from -0.125 to 0.125
- gate_bias: float32 [16], P('tp'), as said below
- w_output: bfloat16 [1024, 2048], P('tp'), may hold values from -0.1875 to 0.1875
Outputs:
- mixed: bfloat16 [32768, 2048], P(('sp', 'tp'))
The draws below stay inside these ranges and needn't reach their ends.
Inputs may be any that keep to these rules, and one draw needn't show every extreme that they name: `gate_bias`: each head's forget gate bias is 4 or more; there is no upper bound.
All inputs are finite; a program needn't handle non-finite values.
Results may differ from the reference program's by a relative error of at most 0.012.
The reference program's roundings to bfloat16 on the way count: a program that leaves them out, or rounds other values in their place, can miss the bound.
Values may be sent and summed in bfloat16 or wider, within the bound.
A program may use at most 64 MiB of HBM per device.

```python
import math
import jax
import jax.numpy as jnp
from jax import lax

D = 2048
HEADS = 16
KV_HEADS = 4
HEAD = 64
TOK_DEV = 256
SEQ = 32768
N_TP = 4


def query_base(base_key):
    raw_values = jax.random.normal(jax.random.fold_in(base_key, 11), (D, HEADS * HEAD), jnp.float32)
    return jnp.clip(raw_values, -5.0, 5.0) / math.sqrt(D)


def draw_w_query(key, part):
    return query_base(key).astype(jnp.bfloat16)


def draw_w_key(key, part):
    raw_values = jax.random.normal(jax.random.fold_in(key, 12), (D, KV_HEADS * HEAD), jnp.float32)
    return (jnp.clip(raw_values, -5.0, 5.0) / math.sqrt(D)).astype(jnp.bfloat16)


def draw_gate_bias(key, part):
    shuffled = jax.random.permutation(jax.random.fold_in(key, 21), HEADS)
    quick = shuffled < HEADS // 2
    lasting = math.log(SEQ) + jax.random.uniform(jax.random.fold_in(key, 22), (HEADS,), jnp.float32, 0.5, 1.5)
    fading = jax.random.uniform(jax.random.fold_in(key, 23), (HEADS,), jnp.float32, 4.1, 5.3)
    return jnp.where(quick, fading, lasting).astype(jnp.float32)


def draw_tokens(key, part):
    span_rows = TOK_DEV // 2
    span_count = SEQ // span_rows
    scales = jnp.exp(jax.random.uniform(jax.random.fold_in(key, 31), (span_count, 1, 1), jnp.float32, math.log(0.6), math.log(1.6)))
    shifts = jax.random.uniform(jax.random.fold_in(key, 32), (span_count, 1, 1), jnp.float32, -1.5, 1.5)
    heading = jnp.clip(jax.random.normal(jax.random.fold_in(key, 33), (1, 1, D), jnp.float32), -3.0, 3.0)
    noise = jnp.clip(jax.random.normal(jax.random.fold_in(key, 34), (span_count, span_rows, D), jnp.float32), -5.0, 5.0)
    field = (scales * (noise + shifts * heading)).reshape(SEQ, D)
    return jnp.clip(field, -16.0, 16.0).astype(jnp.bfloat16)


def block_levels(stream_key, dims, pieces, low, largest):
    loudness = 1.0
    for axis_at, shards_of in pieces:
        steps = jax.random.uniform(jax.random.fold_in(jax.random.fold_in(stream_key, 6), axis_at), (shards_of,), jnp.float32, low / len(pieces), largest / len(pieces))
        loudness = loudness * jnp.repeat(jnp.exp(steps), dims[axis_at] // shards_of).reshape((-1,) + (1,) * (len(dims) - 1 - axis_at))
    return loudness


def normal_values(key, extent, deviation, reach, shards=(), kind=jnp.bfloat16):
    values = jax.random.normal(key, extent, jnp.float32) * deviation
    if len(shards) > 0:
        values = block_levels(key, extent, shards, -0.22, 0.18) * values
    return jnp.clip(values, min=-reach, max=reach).astype(kind)


def setup_inputs(seed: int = 0) -> dict:
    splits = jax.random.split(jax.random.key(seed), 8)
    return {
        "tokens": draw_tokens(jax.random.fold_in(splits[7], 71), 0),
        "w_query": draw_w_query(jax.random.fold_in(splits[7], 71), 0),
        "w_key": draw_w_key(jax.random.fold_in(splits[7], 71), 0),
        "w_value": normal_values(splits[3], (D, KV_HEADS * HEAD), D ** -0.5, 0.125, ((1, 4),)),
        "w_gate": normal_values(splits[4], (D, HEADS), D ** -0.5, 0.125, ((1, 4),)),
        "gate_bias": draw_gate_bias(jax.random.fold_in(splits[7], 71), 0),
        "w_output": normal_values(splits[6], (HEADS * HEAD, D), (HEADS * HEAD) ** -0.5, 0.1875, ((0, 4),)),
    }


masked_value = -1e30


def reference(tokens, w_query, w_key, w_value, w_gate, gate_bias, w_output):
    length = tokens.shape[0]
    group_size = HEADS // KV_HEADS
    queries = jnp.dot(tokens, w_query, preferred_element_type=jnp.float32).astype(jnp.bfloat16)
    key_proj = jnp.dot(tokens, w_key, preferred_element_type=jnp.float32).astype(jnp.bfloat16)
    value_proj = jnp.dot(tokens, w_value, preferred_element_type=jnp.float32).astype(jnp.bfloat16)
    gate_logits = jnp.dot(tokens, w_gate, preferred_element_type=jnp.float32).astype(jnp.bfloat16)
    queries, key_proj, value_proj, gate_logits = lax.optimization_barrier((queries, key_proj, value_proj, gate_logits))
    log_gates = jax.nn.log_sigmoid(gate_logits.astype(jnp.float32) + gate_bias.astype(jnp.float32))
    cumulative = jnp.cumsum(log_gates, axis=0)
    span = math.gcd(length, 512)
    block_total = length // span
    query_all = queries.astype(jnp.float32).reshape(block_total, span, KV_HEADS, group_size, HEAD)
    key_all = key_proj.astype(jnp.float32).reshape(block_total, span, KV_HEADS, HEAD)
    value_all = value_proj.astype(jnp.float32).reshape(block_total, span, KV_HEADS, HEAD)
    cumul_all = cumulative.reshape(block_total, span, KV_HEADS, group_size)
    scale = HEAD ** -0.5

    def query_block(block_index):
        query_here = lax.dynamic_index_in_dim(query_all, block_index, 0, keepdims=False)
        cumul_here = lax.dynamic_index_in_dim(cumul_all, block_index, 0, keepdims=False).transpose(1, 2, 0)
        query_position = block_index * span + jnp.arange(span, dtype=jnp.int32)

        def key_step(key_index, carry_state):
            row_peak, row_mass, row_accum = carry_state
            key_here = lax.dynamic_index_in_dim(key_all, key_index, 0, keepdims=False)
            value_here = lax.dynamic_index_in_dim(value_all, key_index, 0, keepdims=False)
            key_cumul = lax.dynamic_index_in_dim(cumul_all, key_index, 0, keepdims=False).transpose(1, 2, 0)
            key_position = key_index * span + jnp.arange(span, dtype=jnp.int32)
            scores = jnp.einsum("tkgd,skd->kgts", query_here, key_here) * scale
            scores = scores + cumul_here[:, :, :, None] - key_cumul[:, :, None, :]
            allowed = key_position[None, :] <= query_position[:, None]
            scores = jnp.where(allowed, scores, masked_value)
            new_peak = jnp.maximum(row_peak, jnp.max(scores, axis=3))
            weights = jnp.where(allowed, jnp.exp(scores - new_peak[:, :, :, None]), 0.0)
            rescale = jnp.exp(row_peak - new_peak)
            row_mass = row_mass * rescale + jnp.sum(weights, axis=3)
            weights_low = lax.optimization_barrier(weights.astype(jnp.bfloat16))
            row_accum = row_accum * rescale[:, :, :, None] + jnp.einsum(
                "kgts,skd->kgtd", weights_low.astype(jnp.float32), value_here)
            return new_peak, row_mass, row_accum

        initial = (jnp.full((KV_HEADS, group_size, span), masked_value, jnp.float32),
                   jnp.zeros((KV_HEADS, group_size, span), jnp.float32),
                   jnp.zeros((KV_HEADS, group_size, span, HEAD), jnp.float32))
        row_peak, row_mass, row_accum = lax.fori_loop(0, block_index + 1, key_step, initial)
        attended = (row_accum / row_mass[:, :, :, None]).astype(jnp.bfloat16)
        return attended.transpose(2, 0, 1, 3).reshape(span, HEADS * HEAD)

    attended = lax.map(query_block, jnp.arange(block_total, dtype=jnp.int32)).reshape(length, HEADS * HEAD)
    per_group = HEADS * HEAD // N_TP
    total = jnp.zeros((length, D), jnp.float32)
    for group_index in range(N_TP):
        partial_value = jnp.dot(attended[:, group_index * per_group:(group_index + 1) * per_group],
                          w_output[group_index * per_group:(group_index + 1) * per_group],
                          preferred_element_type=jnp.float32).astype(jnp.bfloat16)
        partial_value = lax.optimization_barrier(partial_value)
        total = total + partial_value.astype(jnp.float32)
    return total.astype(jnp.bfloat16)
```

```python
import functools

import jax
import jax.numpy as jnp
from jax import lax
from jax.experimental import pallas as pl
from jax.experimental.pallas import tpu as pltpu
from jax.sharding import PartitionSpec as P

HEAD = 64
LANES = 128
AUG = 16
RING = 8
masked_value = -1e30
skipped_value = -1e38
MESH = pl.DeviceIdType.MESH
f32, bf = jnp.float32, jnp.bfloat16


def pieces_of(x):
    a = x.astype(bf)
    r = x - a.astype(f32)
    b = r.astype(bf)
    c = (r - b.astype(f32)).astype(bf)
    return a, b, c


def kernel(
    sp, tp, ny, chunks,
    tokens, w_query, w_key, w_value, w_gate, bias_in, w_output,
    out,
    tok, wq_raw, wt, w_g, wo_all, proj, kx, qa, own_sum, pair_sum, sums, gk, gq,
    score, weight, tile_max, scaling, peak, acc, x_in, ret_o, ret_s, in_o, in_s,
    att_t, att_out, att_all, bias,
    local_sem, own_sem, ta_send, ta_recv, tb_send, tb_recv,
    sum_send, sum_recv, tot_send, tot_recv,
    q_send, q_recv, pq_send, pq_recv, fq_send, fq_recv,
    z_send, a_send, b_send, kx_recv,
    wa_send, wa_recv, wb_send, wb_recv, wm_send, wm_recv,
    x_send, x_recv, r_send, r_recv, att_send, att_recv,
):
    me = lax.axis_index("sp")
    x = lax.axis_index("tp")
    far_n = sp // 2
    nz = far_n // ny
    deep = nz // 2
    far, side = lax.div(me, 2), lax.rem(me, 2)
    z, y = lax.div(far, ny), lax.rem(far, ny)
    mate = far * 2 + (1 - side)
    sign = 1 - 2 * side
    rows = tok.shape[1]
    local_rows = rows * tp
    width = tok.shape[2]
    q_cols = w_query.shape[1]
    heads = w_gate.shape[0]
    key_cols = w_key.shape[0]
    piece = width // chunks
    kv_at = q_cols
    gate_at = q_cols + 2 * key_cols
    ka_rows = key_cols + AUG
    lanes = heads * local_rows
    out_cols = w_output.shape[1]
    a_hops, b_hops = ny // 2, ny // 2 - 1
    xa_hops, xb_hops = tp // 2, tp // 2 - 1
    heavy = z >= deep
    other_z = nz - 1 - z
    partner_far = other_z * ny + y
    partner = partner_far * 2 + side
    x_a = lax.rem(x + sign + tp, tp)
    x_b = lax.rem(x - sign + tp, tp)
    y_a = (z * ny + lax.rem(y + sign + ny, ny)) * 2 + side
    y_b = (z * ny + lax.rem(y - sign + ny, ny)) * 2 + side

    loads = [
        pltpu.make_async_copy(w_query, wq_raw, local_sem.at[0]),
        pltpu.make_async_copy(w_key, wt.at[pl.ds(kv_at, key_cols)], local_sem.at[1]),
        pltpu.make_async_copy(w_value, wt.at[pl.ds(kv_at + key_cols, key_cols)], local_sem.at[2]),
        pltpu.make_async_copy(w_gate, w_g, local_sem.at[3]),
        pltpu.make_async_copy(bias_in, bias, local_sem.at[4]),
        pltpu.make_async_copy(w_output.at[pl.ds(0, q_cols // 2)], wo_all.at[x, 0], local_sem.at[5]),
        pltpu.make_async_copy(w_output.at[pl.ds(q_cols // 2, q_cols // 2)], wo_all.at[x, 1], local_sem.at[6]),
    ]
    own = pltpu.make_async_copy(tokens, tok.at[x], own_sem)
    own.start()
    for load in loads:
        load.start()

    barrier = pltpu.get_barrier_semaphore()
    for d in range(1, tp):
        pl.semaphore_signal(barrier, inc=1, device_id={"tp": lax.rem(x + d, tp)}, device_id_type=MESH)
    pl.semaphore_signal(barrier, inc=1, device_id={"sp": mate}, device_id_type=MESH)

    def greet(d, carry):
        other = lax.rem(far + d, far_n) * 2 + side
        pl.semaphore_signal(barrier, inc=1, device_id={"sp": other}, device_id_type=MESH)
        return carry

    lax.fori_loop(1, far_n, greet, 0)
    pl.semaphore_wait(barrier, (tp - 1) + 1 + (far_n - 1))

    def remote(src, dst, send, recv, axis, index):
        return pltpu.make_async_remote_copy(
            src, dst, send, recv, device_id={axis: index}, device_id_type=MESH
        )

    def tok_a(d, k):
        ref = tok.at[lax.rem(x - sign * d + tp, tp), :, pl.ds(k * piece, piece)]
        return remote(ref, ref, ta_send.at[d, k], ta_recv.at[d, k], "tp", x_a)

    def tok_b(d, k):
        ref = tok.at[lax.rem(x + sign * d + tp, tp), :, pl.ds(k * piece, piece)]
        return remote(ref, ref, tb_send.at[d, k], tb_recv.at[d, k], "tp", x_b)

    own.wait()
    for k in range(chunks):
        tok_a(0, k).start()
        if xb_hops:
            tok_b(0, k).start()

    for load in loads[:5]:
        load.wait()
    build = 256
    for i in range(width // build):
        wt[0:q_cols, i * build:(i + 1) * build] = wq_raw[i * build:(i + 1) * build, :].T
    wt[gate_at:gate_at + AUG, :] = jnp.concatenate(
        [w_g[...].astype(f32), jnp.zeros((AUG - heads, width), f32)], axis=0
    ).astype(bf)

    q_row = lax.broadcasted_iota(jnp.int32, (AUG, lanes), 0)
    q_head = lax.div(lax.broadcasted_iota(jnp.int32, (AUG, lanes), 1), local_rows)
    pattern = jnp.where(
        (q_row < 3 * heads) & (lax.rem(q_row, heads) == q_head), 1.0, 0.0
    ).astype(bf)
    for i in range(4):
        qa[i, key_cols:ka_rows, :] = pattern

    for k in range(chunks):
        for d in range(1, xa_hops + 1):
            tok_a(d - 1, k).wait_recv()
            if d < xa_hops:
                tok_a(d, k).start()
            if d <= xb_hops:
                tok_b(d - 1, k).wait_recv()
                if d < xb_hops:
                    tok_b(d, k).start()
        here = tok[:, :, k * piece:(k + 1) * piece].reshape(local_rows, piece)
        part = lax.dot_general(
            wt[:, k * piece:(k + 1) * piece], here, (((1,), (1,)), ((), ())),
            preferred_element_type=f32,
        )
        if k == 0:
            proj[...] = part
        else:
            proj[...] += part

    row_of = lax.broadcasted_iota(jnp.int32, (8, local_rows), 0)
    u = proj[gate_at:gate_at + 8, :].astype(bf).astype(f32)
    for h in range(heads):
        u = jnp.where(row_of == h, u + bias[h], u)
    gates = jnp.minimum(u, 0.0) - jnp.log1p(jnp.exp(-jnp.abs(u)))
    gates = jnp.where(row_of < heads, gates, 0.0)
    upper = (
        lax.broadcasted_iota(jnp.int32, (local_rows, local_rows), 0)
        <= lax.broadcasted_iota(jnp.int32, (local_rows, local_rows), 1)
    )
    ones = jnp.where(upper, 1.0, 0.0).astype(bf)
    g0, g1, g2 = pieces_of(gates)
    total = jnp.dot(g2, ones, preferred_element_type=f32)
    total = total + jnp.dot(g1, ones, preferred_element_type=f32)
    total = total + jnp.dot(g0, ones, preferred_element_type=f32)
    own_sum[...] = jnp.broadcast_to(total[:, local_rows - 1:], (8, LANES))
    sum_copy = remote(own_sum, pair_sum, sum_send, sum_recv, "sp", mate)
    sum_copy.start()

    s0, s1, s2 = [p.astype(f32)[:heads] for p in pieces_of(-total)]
    last = jnp.where(lax.broadcasted_iota(jnp.int32, (AUG - 3 * heads, local_rows), 0) == 0, 1.0, 0.0)
    kx[far, 0:key_cols, :] = proj[kv_at:kv_at + key_cols, :].astype(bf)
    kx[far, key_cols:ka_rows, :] = jnp.concatenate([s0, s1, s2, last], axis=0).astype(bf)
    kx[far, ka_rows:, :] = proj[kv_at + key_cols:kv_at + 2 * key_cols, :].astype(bf)

    def ring_a(r):
        return remote(kx.at[r], kx.at[r], a_send.at[r], kx_recv.at[r], "sp", y_a)

    def ring_b(r):
        return remote(kx.at[r], kx.at[r], b_send.at[r], kx_recv.at[r], "sp", y_b)

    def needs(row, at):
        low = jnp.where(at >= deep, at - deep + 1, 0)
        high = jnp.where(at >= deep, at, jnp.maximum(at, deep - 1 - at))
        return (row >= low) & (row <= high)

    def column(d):
        target = lax.rem(z + d, nz)
        return target, remote(
            kx.at[far], kx.at[far], z_send.at[d - 1], kx_recv.at[far],
            "sp", (target * ny + y) * 2 + side,
        )

    ring_a(far).start()
    if b_hops:
        ring_b(far).start()
    for d in range(1, nz):
        target, copy = column(d)

        @pl.when(needs(z, target))
        def _():
            copy.start()

    scale = HEAD ** -0.5
    for h in range(heads):
        qa[side, 0:key_cols, h * local_rows:(h + 1) * local_rows] = (
            proj[h * HEAD:(h + 1) * HEAD, :].astype(bf) * bf(scale)
        )

    q_half = pl.ds(0, key_cols)
    q_copy = remote(qa.at[side, q_half], qa.at[side, q_half], q_send, q_recv, "sp", mate)
    q_copy.start()
    partner_q = remote(qa.at[side, q_half], qa.at[2 + side, q_half], pq_send, pq_recv, "sp", partner)
    forward_q = remote(qa.at[2 + side, q_half], qa.at[2 + side, q_half], fq_send, fq_recv, "sp", mate)

    @pl.when(heavy)
    def _():
        partner_q.start()

    sum_copy.wait_recv()
    start_rep = jnp.where(side == 1, pair_sum[...], 0.0)
    both = own_sum[...] + pair_sum[...]
    pick = (
        lax.broadcasted_iota(jnp.int32, (8, LANES), 0)
        == lax.div(lax.broadcasted_iota(jnp.int32, (8, LANES), 1), LANES // heads)
    )
    sums[far] = jnp.concatenate(
        [
            jnp.sum(jnp.where(pick, both, 0.0), axis=0, keepdims=True),
            jnp.sum(jnp.where(pick, start_rep, 0.0), axis=0, keepdims=True),
        ],
        axis=1,
    )

    def tell(d):
        return remote(
            sums.at[far], sums.at[far], tot_send.at[d], tot_recv.at[far],
            "sp", lax.rem(far + d, far_n) * 2 + side,
        )

    def hear(d):
        r = lax.rem(far + d, far_n)
        return remote(sums.at[r], sums.at[r], tot_send.at[d], tot_recv.at[r], "sp", r * 2 + side)

    def send_total(d, carry):
        tell(d).start()
        return carry

    lax.fori_loop(1, far_n, send_total, 0)

    for load in loads[5:]:
        load.wait()

    def wo_a(d):
        ref = wo_all.at[lax.rem(x - sign * d + tp, tp), side]
        return remote(ref, ref, wa_send.at[d], wa_recv.at[d], "tp", x_a)

    def wo_b(d):
        ref = wo_all.at[lax.rem(x + sign * d + tp, tp), side]
        return remote(ref, ref, wb_send.at[d], wb_recv.at[d], "tp", x_b)

    def wo_mate(d):
        ref = wo_all.at[lax.rem(x + d, tp), side]
        return remote(ref, ref, wm_send.at[d - 1], wm_recv.at[d - 1], "sp", mate)

    wo_a(0).start()
    if xb_hops:
        wo_b(0).start()

    def doubled(row, h):
        part = row[:, h * LANES:(h + 1) * LANES]
        return jnp.concatenate([part] * (local_rows // LANES), axis=1)

    q_copy.wait_recv()
    key_at = lax.broadcasted_iota(jnp.int32, (local_rows, local_rows), 0) + side * local_rows
    query_at = lax.broadcasted_iota(jnp.int32, (local_rows, local_rows), 1)
    ka = kx[far, 0:ka_rows, :].T
    va = kx[far, key_cols:, :]
    for g in range(2):
        allowed = key_at <= query_at + g * local_rows
        for h in range(heads):
            here = slice(h * local_rows, (h + 1) * local_rows)
            s = jnp.dot(ka, qa[g, :, here], preferred_element_type=f32)
            shift = jnp.concatenate([start_rep[h:h + 1]] * (local_rows // LANES), axis=1)
            s = jnp.where(allowed, s - shift, masked_value)
            top = jnp.max(s, axis=0, keepdims=True)
            peak[g, :, here] = top
            acc[g, :, here] = jnp.dot(va, jnp.exp(s - top).astype(bf), preferred_element_type=f32)
    peak[2:4] = jnp.full((2, 1, lanes), masked_value, f32)
    acc[2:4] = jnp.zeros((2,) + acc.shape[1:], f32)
    weight[1] = jnp.zeros(weight.shape[1:], bf)
    scaling[1] = jnp.ones(scaling.shape[1:], f32)

    def hear_total(d, carry):
        hear(d).wait_recv()
        return carry

    lax.fori_loop(1, far_n, hear_total, 0)
    lower = (
        lax.broadcasted_iota(jnp.int32, (far_n, far_n), 1)
        < lax.broadcasted_iota(jnp.int32, (far_n, far_n), 0)
    )
    below = jnp.where(lower, 1.0, 0.0).astype(bf)
    table = sums[...].reshape(far_n, 2 * LANES)
    t0, t1, t2 = pieces_of(table[:, :LANES])
    before = jnp.dot(below, t2, preferred_element_type=f32)
    before = before + jnp.dot(below, t1, preferred_element_type=f32)
    before = before + jnp.dot(below, t0, preferred_element_type=f32)
    starts = before + table[:, LANES:]
    for h in range(heads):
        at = h * (LANES // heads)
        span = slice(h * LANES, (h + 1) * LANES)
        gq[:, span] = jnp.broadcast_to(before[:, at:at + 1], (far_n, LANES))
        gk[:, span] = jnp.broadcast_to(starts[:, at:at + 1], (far_n, LANES))

    per = jnp.where(heavy, deep, deep + 1)
    items = per * ny

    def item(n):
        step, j = lax.div(n, per), lax.rem(n, per)
        mine = j <= z
        row = jnp.where(mine, z - j, j - z - 1)
        d = lax.div(step + 1, 2)
        odd = lax.rem(step, 2)
        source = lax.rem(y + jnp.where(odd == 1, -d, d) * sign + ny, ny)
        r = row * ny + source
        skip = mine & (row == z) & (source >= y)
        first = mine | (row > z)
        along_a = ((step == 0) | (odd == 1)) & (d < a_hops)
        along_b = (odd == 0) & (d < b_hops)
        return r, jnp.where(mine, 0, 1), skip, first, along_a, along_b

    def arrive(n):
        r, _, _, first, along_a, along_b = item(n)

        @pl.when(first & (r != far))
        def _():
            ring_a(r).wait_recv()

            @pl.when(along_a)
            def _():
                ring_a(r).start()

            @pl.when(along_b)
            def _():
                ring_b(r).start()

        if nz > 1:
            light = jnp.logical_not(heavy)

            @pl.when(light & (n == 0))
            def _():
                partner_q.wait_recv()
                forward_q.start()

            @pl.when(light & (n == z + 1))
            def _():
                forward_q.wait_recv()

    def score_stage(n, b):
        r, q, _, _, _, _ = item(n)
        ka = kx[r, 0:ka_rows, :].T

        def run(g, here):
            s = jnp.dot(ka, qa[2 * q + g, :, here], preferred_element_type=f32)
            score[b, g, :, here] = s
            tile_max[b, g, :, here] = jnp.max(s, axis=0, keepdims=True)

        return run

    def weight_stage(n, b):
        r, q, skip, _, _, _ = item(n)
        chip = jnp.where(q == 0, far, partner_far)
        offset = gq[pl.ds(chip, 1), :] - gk[pl.ds(r, 1), :]
        offset = jnp.where(skip, skipped_value, offset)

        def run(g, here, h):
            o = doubled(offset, h)
            old = peak[2 * q + g, :, here]
            new = jnp.maximum(old, tile_max[b, g, :, here] + o)
            weight[b, g, :, here] = jnp.exp(score[b, g, :, here] - (new - o)).astype(bf)
            scaling[b, g, :, here] = jnp.exp(old - new)
            peak[2 * q + g, :, here] = new

        return run

    def sum_stage(n, b):
        r, q, _, _, _, _ = item(n)
        va = kx[r, key_cols:, :]

        def run(g, here):
            term = jnp.dot(va, weight[b, g, :, here], preferred_element_type=f32)
            acc[2 * q + g, :, here] = acc[2 * q + g, :, here] * scaling[b, g, :, here] + term

        return run

    tiles = [(g, h, slice(h * local_rows, (h + 1) * local_rows)) for g in range(2) for h in range(heads)]
    arrive(jnp.int32(0))
    begin = score_stage(jnp.int32(0), 0)
    for g, h, here in tiles:
        begin(g, here)

    def trip(i, carry):
        n = 2 * i

        @pl.when(n + 1 < items)
        def _():
            arrive(n + 1)

        @pl.when(n + 2 < items)
        def _():
            arrive(n + 2)

        @pl.when(i == lax.div(items, 4))
        def _():
            wo_a(0).wait_recv()
            if xa_hops > 1:
                wo_a(1).start()
            if xb_hops:
                wo_b(0).wait_recv()

        @pl.when(i == lax.div(items * 7, 16))
        def _():
            if xa_hops > 1:
                wo_a(1).wait_recv()
            for d in range(1, tp):
                wo_mate(d).start()

        for b in range(2):
            now = n + b
            scores = score_stage(jnp.minimum(now + 1, items - 1), 1 - b)
            weights = weight_stage(now, b)
            terms = sum_stage(jnp.maximum(now - 1, 0), 1 - b)
            for g, h, here in tiles:
                scores(g, here)
                weights(g, here, h)
                terms(g, here)
        return carry

    lax.fori_loop(0, lax.div(items, 2), trip, 0)
    finish = sum_stage(items - 1, 1)
    for g, h, here in tiles:
        finish(g, here)

    mass_at, peak_at = 3 * heads, 3 * heads + 1
    cut = 8

    def to_mate(q):
        return remote(
            acc.at[2 * q + 1 - side, pl.ds(cut, ka_rows - cut)], x_in.at[q],
            x_send.at[q], x_recv.at[q], "sp", mate,
        )

    def merged(q):
        mine = 2 * q + side
        a_mass, a_peak = acc[mine, mass_at:mass_at + 1, :], peak[mine]
        b_mass, b_peak = x_in[q, mass_at - cut:mass_at - cut + 1, :], x_in[q, peak_at - cut:peak_at - cut + 1, :]
        top = jnp.maximum(a_peak, b_peak)
        wa, wb = jnp.exp(a_peak - top), jnp.exp(b_peak - top)
        return top, a_mass * wa + b_mass * wb, wa, wb

    def sums_of(q, wa, wb, here):
        return (
            acc[2 * q + side, AUG:, here] * wa[:, here] + x_in[q, AUG - cut:, here] * wb[:, here]
        )

    for q in range(2):
        acc[2 * q + 1 - side, peak_at:peak_at + 1, :] = peak[2 * q + 1 - side]
    ret_copies = [
        remote(ret_o, in_o, r_send.at[0], r_recv.at[0], "sp", partner),
        remote(ret_s, in_s, r_send.at[1], r_recv.at[1], "sp", partner),
    ]

    @pl.when(jnp.logical_not(heavy))
    def _():
        to_mate(1).start()
        to_mate(0).start()
        to_mate(1).wait_recv()
        top, mass, wa, wb = merged(1)
        inverse = 1.0 / mass
        for h in range(heads):
            here = slice(h * local_rows, (h + 1) * local_rows)
            ret_o[:, here] = (sums_of(1, wa, wb, here) * inverse[:, here]).astype(bf)
        ret_s[0:1, :] = top
        ret_s[1:2, :] = mass
        for copy in ret_copies:
            copy.start()
        to_mate(0).wait_recv()
        top, mass, wa, wb = merged(0)
        inverse = 1.0 / mass
        for h in range(heads):
            here = slice(h * local_rows, (h + 1) * local_rows)
            att_t[h * HEAD:(h + 1) * HEAD, :] = (sums_of(0, wa, wb, here) * inverse[:, here]).astype(bf)

    @pl.when(heavy)
    def _():
        to_mate(0).start()
        to_mate(0).wait_recv()
        top, mass, wa, wb = merged(0)
        for copy in ret_copies:
            copy.wait_recv()
        r_top, r_mass = in_s[0:1, :], in_s[1:2, :]
        best = jnp.maximum(top, r_top)
        w_own, w_far = jnp.exp(top - best), jnp.exp(r_top - best) * r_mass
        inverse = 1.0 / (mass * w_own + w_far)
        w_own, w_far = w_own * inverse, w_far * inverse
        for h in range(heads):
            here = slice(h * local_rows, (h + 1) * local_rows)
            att_t[h * HEAD:(h + 1) * HEAD, :] = (
                sums_of(0, wa, wb, here) * w_own[:, here] + in_o[:, here].astype(f32) * w_far[:, here]
            ).astype(bf)

    att_out[...] = att_t[...].T.reshape(tp, rows, q_cols)

    def att_copy(d):
        to = lax.rem(x + d, tp)
        return remote(att_out.at[to], att_all.at[x], att_send.at[d - 1], att_recv.at[d - 1], "tp", to)

    for d in range(1, tp):
        att_copy(d).start()
    att_all[x] = att_out[x]
    for d in range(1, tp):
        wo_mate(d).wait_recv()
    for d in range(1, tp):
        att_copy(d).wait_recv()
    for k in range(4):
        span = slice(k * (out_cols // 4), (k + 1) * (out_cols // 4))
        value = None
        for r in range(tp):
            term = jnp.dot(
                att_all[r], wo_all[r, :, :, span].reshape(q_cols, out_cols // 4),
                preferred_element_type=f32,
            ).astype(bf).astype(f32)
            value = term if value is None else value + term
        out[:, span] = value.astype(bf)

    for k in range(chunks):
        for d in range(xa_hops):
            tok_a(d, k).wait_send()
        for d in range(xb_hops):
            tok_b(d, k).wait_send()
    sum_copy.wait_send()
    q_copy.wait_send()

    def drain_total(d, carry):
        tell(d).wait_send()
        return carry

    lax.fori_loop(1, far_n, drain_total, 0)
    for d in range(xa_hops):
        wo_a(d).wait_send()
    for d in range(xb_hops):
        wo_b(d).wait_send()
    for d in range(1, tp):
        wo_mate(d).wait_send()
        att_copy(d).wait_send()
    for d in range(1, nz):
        target, copy = column(d)

        @pl.when(needs(z, target))
        def _():
            copy.wait_send()

    def drain(n, carry):
        r, _, _, first, along_a, along_b = item(n)

        @pl.when(first & along_a)
        def _():
            ring_a(r).wait_send()

        @pl.when(first & along_b)
        def _():
            ring_b(r).wait_send()

        return carry

    lax.fori_loop(0, items, drain, 0)
    to_mate(0).wait_send()

    @pl.when(heavy)
    def _():
        partner_q.wait_send()

    @pl.when(jnp.logical_not(heavy))
    def _():
        forward_q.wait_send()
        to_mate(1).wait_send()
        for copy in ret_copies:
            copy.wait_send()


def shards(ny, tokens, w_query, w_key, w_value, w_gate, gate_bias, w_output):
    sp = lax.axis_size("sp")
    tp = lax.axis_size("tp")
    rows, width = tokens.shape
    local_rows = rows * tp
    q_cols, key_cols, heads = w_query.shape[1], w_key.shape[1], w_gate.shape[1]
    out_cols = w_output.shape[1]
    assert key_cols == HEAD and heads == 4 and q_cols == heads * HEAD
    chunks = 4 if width % 512 == 0 else 2
    far_n = sp // 2
    nz = far_n // ny
    lanes = heads * local_rows
    ka_rows = key_cols + AUG
    xa, xb = tp // 2, max(tp // 2 - 1, 1)
    dma = pltpu.SemaphoreType.DMA
    hbm_spec = pl.BlockSpec(memory_space=pltpu.HBM)
    vmem_spec = pl.BlockSpec(memory_space=pltpu.VMEM)
    operands = (tokens, w_query, w_key.T, w_value.T, w_gate.T, gate_bias, w_output)
    vmem = pltpu.VMEM
    return pl.pallas_call(
        functools.partial(kernel, sp, tp, ny, chunks),
        out_shape=jax.ShapeDtypeStruct((rows, out_cols), bf),
        in_specs=[hbm_spec] * 7,
        out_specs=vmem_spec,
        scratch_shapes=[
            vmem((tp, rows, width), bf),
            vmem((width, q_cols), bf),
            vmem((q_cols + 2 * key_cols + AUG, width), bf),
            vmem((heads, width), bf),
            vmem((tp, 2, q_cols // 2, out_cols), bf),
            vmem((q_cols + 2 * key_cols + AUG, local_rows), f32),
            vmem((far_n, ka_rows + key_cols, local_rows), bf),
            vmem((4, ka_rows, lanes), bf),
            vmem((8, LANES), f32),
            vmem((8, LANES), f32),
            vmem((far_n, 1, 2 * LANES), f32),
            vmem((far_n, heads * LANES), f32),
            vmem((far_n, heads * LANES), f32),
            vmem((2, 2, local_rows, lanes), f32),
            vmem((2, 2, local_rows, lanes), bf),
            vmem((2, 2, 1, lanes), f32),
            vmem((2, 2, 1, lanes), f32),
            vmem((4, 1, lanes), f32),
            vmem((4, ka_rows, lanes), f32),
            vmem((2, ka_rows - 8, lanes), f32),
            vmem((key_cols, lanes), bf),
            vmem((8, lanes), f32),
            vmem((key_cols, lanes), bf),
            vmem((8, lanes), f32),
            vmem((q_cols, local_rows), bf),
            vmem((tp, rows, q_cols), bf),
            vmem((tp, rows, q_cols), bf),
            pltpu.SMEM((heads,), f32),
            dma((7,)),
            dma,
            dma((xa, chunks)),
            dma((xa, chunks)),
            dma((xb, chunks)),
            dma((xb, chunks)),
            dma,
            dma,
            dma((far_n,)),
            dma((far_n,)),
            dma,
            dma,
            dma,
            dma,
            dma,
            dma,
            dma((nz,)),
            dma((far_n,)),
            dma((far_n,)),
            dma((far_n,)),
            dma((xa,)),
            dma((xa,)),
            dma((xb,)),
            dma((xb,)),
            dma((tp - 1,)),
            dma((tp - 1,)),
            dma((2,)),
            dma((2,)),
            dma((2,)),
            dma((2,)),
            dma((tp - 1,)),
            dma((tp - 1,)),
        ],
        compiler_params=pltpu.CompilerParams(
            collective_id=0, has_side_effects=True, vmem_limit_bytes=60 << 20
        ),
    )(*(pltpu.with_memory_space_constraint(x, pltpu.HBM) for x in operands))


def solution(mesh):
    return jax.shard_map(
        functools.partial(shards, min(RING, mesh.shape["sp"] // 4)),
        mesh=mesh,
        in_specs=(
            P(("sp", "tp"), None),
            P(None, "tp"),
            P(None, "tp"),
            P(None, "tp"),
            P(None, "tp"),
            P("tp"),
            P("tp", None),
        ),
        out_specs=P(("sp", "tp"), None),
        check_vma=False,
    )
```

```python
import functools

import jax
import jax.numpy as jnp
from jax import lax
from jax.experimental import pallas as pl
from jax.experimental.pallas import tpu as pltpu
from jax.sharding import PartitionSpec as P

HEAD = 64
LANES = 128
AUG = 16
RING = 8
CUT = 8
MASS, PEAK = 12 - CUT, 13 - CUT
masked_value = -1e30
skipped_value = -1e38
MESH = pl.DeviceIdType.MESH
f32, bf = jnp.float32, jnp.bfloat16


def pieces_of(x):
    a = x.astype(bf)
    r = x - a.astype(f32)
    b = r.astype(bf)
    c = (r - b.astype(f32)).astype(bf)
    return a, b, c


def kernel(
    sp, tp, ny, chunks,
    tokens, w_query, w_key, w_value, w_gate, bias_in, w_output,
    out,
    tok, wq_raw, wt, w_g, wo_all, proj, kx, qa, sums, pair_sums, gk, gq,
    score, tile_max, peak, acc, x_in, ret_o, ret_s, in_o, in_s,
    att_t, att_out, att_all, bias,
    local_sem, own_sem, ta_send, ta_recv, tb_send, tb_recv,
    sum_send, sum_recv, tot_send, tot_recv,
    q_send, q_recv, pq_send, pq_recv, fq_send, fq_recv,
    z_send, a_send, b_send, kx_recv,
    wa_send, wa_recv, wb_send, wb_recv, wm_send, wm_recv,
    x_send, x_recv, r_send, r_recv, att_send, att_recv,
):
    me = lax.axis_index("sp")
    x = lax.axis_index("tp")
    far_n = sp // 2
    nz = far_n // ny
    deep = nz // 2
    far, side = lax.div(me, 2), lax.rem(me, 2)
    z, y = lax.div(far, ny), lax.rem(far, ny)
    mate = far * 2 + (1 - side)
    sign = 1 - 2 * side
    rows = tok.shape[1]
    local_rows = rows * tp
    width = tok.shape[2]
    q_cols = w_query.shape[1]
    heads = w_gate.shape[0]
    key_cols = w_key.shape[0]
    piece = width // chunks
    kv_at = q_cols
    gate_at = q_cols + 2 * key_cols
    ka_rows = key_cols + AUG
    lanes = heads * local_rows
    out_cols = w_output.shape[1]
    a_hops, b_hops = ny // 2, ny // 2 - 1
    xa_hops, xb_hops = tp // 2, tp // 2 - 1
    heavy = z >= deep
    other_z = nz - 1 - z
    partner_far = other_z * ny + y
    partner = partner_far * 2 + side
    x_a = lax.rem(x + sign + tp, tp)
    x_b = lax.rem(x - sign + tp, tp)
    y_a = (z * ny + lax.rem(y + sign + ny, ny)) * 2 + side
    y_b = (z * ny + lax.rem(y - sign + ny, ny)) * 2 + side

    loads = [
        pltpu.make_async_copy(w_query, wq_raw, local_sem.at[0]),
        pltpu.make_async_copy(w_key, wt.at[pl.ds(kv_at, key_cols)], local_sem.at[1]),
        pltpu.make_async_copy(w_value, wt.at[pl.ds(kv_at + key_cols, key_cols)], local_sem.at[2]),
        pltpu.make_async_copy(w_gate, w_g, local_sem.at[3]),
        pltpu.make_async_copy(bias_in, bias, local_sem.at[4]),
        pltpu.make_async_copy(w_output.at[pl.ds(0, q_cols // 2)], wo_all.at[x, 0], local_sem.at[5]),
        pltpu.make_async_copy(w_output.at[pl.ds(q_cols // 2, q_cols // 2)], wo_all.at[x, 1], local_sem.at[6]),
    ]
    own = pltpu.make_async_copy(tokens, tok.at[x], own_sem)
    own.start()
    for load in loads:
        load.start()

    barrier = pltpu.get_barrier_semaphore()
    for d in range(1, tp):
        pl.semaphore_signal(barrier, inc=1, device_id={"tp": lax.rem(x + d, tp)}, device_id_type=MESH)
    pl.semaphore_signal(barrier, inc=1, device_id={"sp": mate}, device_id_type=MESH)

    def greet(d, carry):
        other = lax.rem(far + d, far_n) * 2 + side
        pl.semaphore_signal(barrier, inc=1, device_id={"sp": other}, device_id_type=MESH)
        return carry

    lax.fori_loop(1, far_n, greet, 0)
    pl.semaphore_wait(barrier, (tp - 1) + 1 + (far_n - 1))

    def remote(src, dst, send, recv, axis, index):
        return pltpu.make_async_remote_copy(
            src, dst, send, recv, device_id={axis: index}, device_id_type=MESH
        )

    def tok_a(d, k):
        ref = tok.at[lax.rem(x - sign * d + tp, tp), :, pl.ds(k * piece, piece)]
        return remote(ref, ref, ta_send.at[d, k], ta_recv.at[d, k], "tp", x_a)

    def tok_b(d, k):
        ref = tok.at[lax.rem(x + sign * d + tp, tp), :, pl.ds(k * piece, piece)]
        return remote(ref, ref, tb_send.at[d, k], tb_recv.at[d, k], "tp", x_b)

    own.wait()
    for k in range(chunks):
        tok_a(0, k).start()
        if xb_hops:
            tok_b(0, k).start()

    for load in loads[:5]:
        load.wait()
    build = 256
    for i in range(width // build):
        wt[0:q_cols, i * build:(i + 1) * build] = wq_raw[i * build:(i + 1) * build, :].T
    wt[gate_at:gate_at + AUG, :] = jnp.concatenate(
        [w_g[...].astype(f32), jnp.zeros((AUG - heads, width), f32)], axis=0
    ).astype(bf)

    q_row = lax.broadcasted_iota(jnp.int32, (AUG, lanes), 0)
    q_head = lax.div(lax.broadcasted_iota(jnp.int32, (AUG, lanes), 1), local_rows)
    pattern = jnp.where(
        (q_row < 3 * heads) & (lax.rem(q_row, heads) == q_head), 1.0, 0.0
    ).astype(bf)
    for i in range(4):
        qa[i, key_cols:ka_rows, :] = pattern

    def relay(d, k):
        tok_a(d - 1, k).wait_recv()
        if d < xa_hops:
            tok_a(d, k).start()
        if d <= xb_hops:
            tok_b(d - 1, k).wait_recv()
            if d < xb_hops:
                tok_b(d, k).start()

    for d in range(1, xa_hops):
        for k in range(chunks):
            relay(d, k)
    for k in range(chunks):
        relay(xa_hops, k)
        here = tok[:, :, k * piece:(k + 1) * piece].reshape(local_rows, piece)
        part = lax.dot_general(
            wt[:, k * piece:(k + 1) * piece], here, (((1,), (1,)), ((), ())),
            preferred_element_type=f32,
        )
        if k == 0:
            proj[...] = part
        else:
            proj[...] += part

    row_of = lax.broadcasted_iota(jnp.int32, (8, local_rows), 0)
    u = proj[gate_at:gate_at + 8, :].astype(bf).astype(f32)
    for h in range(heads):
        u = jnp.where(row_of == h, u + bias[h], u)
    gates = jnp.minimum(u, 0.0) - jnp.log1p(jnp.exp(-jnp.abs(u)))
    gates = jnp.where(row_of < heads, gates, 0.0)
    upper = (
        lax.broadcasted_iota(jnp.int32, (local_rows, local_rows), 0)
        <= lax.broadcasted_iota(jnp.int32, (local_rows, local_rows), 1)
    )
    ones = jnp.where(upper, 1.0, 0.0).astype(bf)
    g0, g1, g2 = pieces_of(gates)
    total = jnp.dot(g2, ones, preferred_element_type=f32)
    total = total + jnp.dot(g1, ones, preferred_element_type=f32)
    total = total + jnp.dot(g0, ones, preferred_element_type=f32)
    pick = (
        lax.broadcasted_iota(jnp.int32, (8, LANES), 0)
        == lax.div(lax.broadcasted_iota(jnp.int32, (8, LANES), 1), LANES // heads)
    )
    block_sum = jnp.broadcast_to(total[:, local_rows - 1:], (8, LANES))
    sums[far] = jnp.sum(jnp.where(pick, block_sum, 0.0), axis=0, keepdims=True)

    def tell(d):
        return remote(
            sums.at[far], sums.at[far], tot_send.at[d], tot_recv.at[far],
            "sp", lax.rem(far + d, far_n) * 2 + side,
        )

    def hear(d):
        r = lax.rem(far + d, far_n)
        return remote(sums.at[r], sums.at[r], tot_send.at[d], tot_recv.at[r], "sp", r * 2 + side)

    def send_total(d, carry):
        tell(d).start()
        return carry

    lax.fori_loop(1, far_n, send_total, 0)

    s0, s1, s2 = [p.astype(f32)[:heads] for p in pieces_of(-total)]
    last = jnp.where(lax.broadcasted_iota(jnp.int32, (AUG - 3 * heads, local_rows), 0) == 0, 1.0, 0.0)
    kx[far, 0:key_cols, :] = proj[kv_at:kv_at + key_cols, :].astype(bf)
    kx[far, key_cols:ka_rows, :] = jnp.concatenate([s0, s1, s2, last], axis=0).astype(bf)
    kx[far, ka_rows:, :] = proj[kv_at + key_cols:kv_at + 2 * key_cols, :].astype(bf)

    def ring_a(r):
        return remote(kx.at[r], kx.at[r], a_send.at[r], kx_recv.at[r], "sp", y_a)

    def ring_b(r):
        return remote(kx.at[r], kx.at[r], b_send.at[r], kx_recv.at[r], "sp", y_b)

    def needs(row, at):
        low = jnp.where(at >= deep, at - deep + 1, 0)
        high = jnp.where(at >= deep, at, jnp.maximum(at, deep - 1 - at))
        return (row >= low) & (row <= high)

    def column(d):
        target = lax.rem(z + d, nz)
        return target, remote(
            kx.at[far], kx.at[far], z_send.at[d - 1], kx_recv.at[far],
            "sp", (target * ny + y) * 2 + side,
        )

    ring_a(far).start()
    if b_hops:
        ring_b(far).start()
    for d in range(1, nz):
        target, copy = column(d)

        @pl.when(needs(z, target))
        def _():
            copy.start()

    scale = HEAD ** -0.5
    for h in range(heads):
        qa[side, 0:key_cols, h * local_rows:(h + 1) * local_rows] = (
            proj[h * HEAD:(h + 1) * HEAD, :].astype(bf) * bf(scale)
        )

    q_half = pl.ds(0, key_cols)
    q_copy = remote(qa.at[side, q_half], qa.at[side, q_half], q_send, q_recv, "sp", mate)
    q_copy.start()
    partner_q = remote(qa.at[side, q_half], qa.at[2 + side, q_half], pq_send, pq_recv, "sp", partner)
    forward_q = remote(qa.at[2 + side, q_half], qa.at[2 + side, q_half], fq_send, fq_recv, "sp", mate)

    @pl.when(heavy)
    def _():
        partner_q.start()

    for load in loads[5:]:
        load.wait()

    def wo_a(d):
        ref = wo_all.at[lax.rem(x - sign * d + tp, tp), side]
        return remote(ref, ref, wa_send.at[d], wa_recv.at[d], "tp", x_a)

    def wo_b(d):
        ref = wo_all.at[lax.rem(x + sign * d + tp, tp), side]
        return remote(ref, ref, wb_send.at[d], wb_recv.at[d], "tp", x_b)

    def wo_mate(d):
        ref = wo_all.at[lax.rem(x + d, tp), side]
        return remote(ref, ref, wm_send.at[d - 1], wm_recv.at[d - 1], "sp", mate)

    wo_a(0).start()
    if xb_hops:
        wo_b(0).start()

    def doubled(row, h):
        part = row[:, h * LANES:(h + 1) * LANES]
        return jnp.concatenate([part] * (local_rows // LANES), axis=1)

    q_copy.wait_recv()
    key_at = lax.broadcasted_iota(jnp.int32, (local_rows, local_rows), 0) + side * local_rows
    query_at = lax.broadcasted_iota(jnp.int32, (local_rows, local_rows), 1)
    ka = kx[far, 0:ka_rows, :].T
    va = kx[far, key_cols:, :]
    for g in range(2):
        allowed = key_at <= query_at + g * local_rows
        for h in range(heads):
            here = slice(h * local_rows, (h + 1) * local_rows)
            s = jnp.dot(ka, qa[g, :, here], preferred_element_type=f32)
            s = jnp.where(allowed, s, masked_value)
            top = jnp.max(s, axis=0, keepdims=True)
            peak[g, :, here] = top
            term = jnp.dot(va, jnp.exp(s - top).astype(bf), preferred_element_type=f32)
            acc[g, :, here] = term[CUT:]
    peak[2:4] = jnp.full((2, 1, lanes), masked_value, f32)
    acc[2:4] = jnp.zeros((2,) + acc.shape[1:], f32)

    top_row = jnp.where(heavy, z, jnp.maximum(z, other_z - deep))
    row_n = jnp.where(heavy, deep, top_row + 1)

    def event(e):
        step, at = lax.div(e, row_n), lax.rem(e, row_n)
        d = lax.div(step + 1, 2)
        odd = lax.rem(step, 2)
        source = lax.rem(y + jnp.where(odd == 1, -d, d) * sign + ny, ny)
        along_a = ((step == 0) | (odd == 1)) & (d < a_hops)
        along_b = (odd == 0) & (d < b_hops)
        return (top_row - at) * ny + source, along_a, along_b

    def arrive(e, carry):
        r, along_a, along_b = event(e)

        @pl.when(r != far)
        def _():
            ring_a(r).wait_recv()

            @pl.when(along_a)
            def _():
                ring_a(r).start()

            @pl.when(along_b)
            def _():
                ring_b(r).start()

        return carry

    lax.fori_loop(0, row_n, arrive, 0)

    def hear_total(d, carry):
        hear(d).wait_recv()
        return carry

    lax.fori_loop(1, far_n, hear_total, 0)
    sum_copy = remote(sums, pair_sums, sum_send, sum_recv, "sp", mate)
    sum_copy.start()
    lower = (
        lax.broadcasted_iota(jnp.int32, (far_n, far_n), 1)
        < lax.broadcasted_iota(jnp.int32, (far_n, far_n), 0)
    )
    below = jnp.where(lower, 1.0, 0.0).astype(bf)
    sum_copy.wait_recv()
    pair_table = pair_sums[...].reshape(far_n, LANES)
    start_table = jnp.where(side == 1, pair_table, 0.0)
    t0, t1, t2 = pieces_of(sums[...].reshape(far_n, LANES) + pair_table)
    before = jnp.dot(below, t2, preferred_element_type=f32)
    before = before + jnp.dot(below, t1, preferred_element_type=f32)
    before = before + jnp.dot(below, t0, preferred_element_type=f32)
    starts = before + start_table
    for h in range(heads):
        at = h * (LANES // heads)
        span = slice(h * LANES, (h + 1) * LANES)
        gq[:, span] = jnp.broadcast_to(before[:, at:at + 1], (far_n, LANES))
        gk[:, span] = jnp.broadcast_to(starts[:, at:at + 1], (far_n, LANES))

    own_shift = gq[pl.ds(far, 1), :] - gk[pl.ds(far, 1), :]
    for g in range(2):
        for h in range(heads):
            here = slice(h * local_rows, (h + 1) * local_rows)
            peak[g, :, here] = peak[g, :, here] + doubled(own_shift, h)

    lent = jnp.where(heavy, 0, other_z - deep + 1)
    kept = jnp.where(heavy, deep, z + 1)
    lag = jnp.where(heavy, 0, min(2, ny - 1))
    per = kept + lent
    head_items = lag * lent
    core_items = (ny - lag) * per
    items = per * ny
    partner_items = jnp.where(heavy, items, head_items + core_items - kept)

    def item(n):
        in_head = n < head_items
        in_core = n < head_items + core_items
        m = jnp.where(in_head, n, jnp.where(in_core, n - head_items, n - head_items - core_items))
        group = jnp.where(in_head, jnp.maximum(lent, 1), jnp.where(in_core, per, kept))
        t, j = lax.div(m, group), lax.rem(m, group)
        borrowed = in_head | (in_core & (j < lent))
        k = jnp.where(borrowed, j, jnp.where(in_core, j - lent, j))
        arrived = jnp.where(in_head, t, jnp.where(in_core, t + lag, ny))
        step = jnp.where(borrowed, arrived, jnp.where(in_core, t, t + ny - lag))
        row = jnp.where(borrowed, other_z - deep - k, z - k)
        d = lax.div(step + 1, 2)
        odd = lax.rem(step, 2)
        source = lax.rem(y + jnp.where(odd == 1, -d, d) * sign + ny, ny)
        skip = jnp.logical_not(borrowed) & (row == z) & (source >= y)
        exact = borrowed | heavy
        need = jnp.where(
            exact, arrived * row_n + top_row - row + 1, jnp.minimum(arrived + 1, ny) * row_n
        )
        return row * ny + source, jnp.where(borrowed, 1, 0), skip, jnp.maximum(need, row_n)

    def score_stage(n, b):
        r, q, _, _ = item(n)
        ka = kx[r, 0:ka_rows, :].T

        def run(g, here):
            s = jnp.dot(ka, qa[2 * q + g, :, here], preferred_element_type=f32)
            score[b, g, :, here] = s
            tile_max[b, g, :, here] = jnp.max(s, axis=0, keepdims=True)

        return run

    def sum_stage(n, b):
        r, q, skip, _ = item(n)
        va = kx[r, key_cols:, :]
        chip = jnp.where(q == 0, far, partner_far)
        offset = gq[pl.ds(chip, 1), :] - gk[pl.ds(r, 1), :]
        offset = jnp.where(skip, skipped_value, offset)

        def run(g, here, h):
            o = doubled(offset, h)
            old = peak[2 * q + g, :, here]
            new = jnp.maximum(old, tile_max[b, g, :, here] + o)
            weight = jnp.exp(score[b, g, :, here] - (new - o)).astype(bf)
            rescale = jnp.exp(old - new)
            peak[2 * q + g, :, here] = new
            term = jnp.dot(va, weight, preferred_element_type=f32)
            acc[2 * q + g, :, here] = acc[2 * q + g, :, here] * rescale + term[CUT:]

        return run

    tiles = [(g, h, slice(h * local_rows, (h + 1) * local_rows)) for g in range(2) for h in range(heads)]

    @pl.when(jnp.logical_not(heavy))
    def _():
        partner_q.wait_recv()
        forward_q.start()
        forward_q.wait_recv()

    lax.fori_loop(row_n, item(jnp.int32(0))[3], arrive, 0)
    begin = score_stage(jnp.int32(0), 0)
    for g, h, here in tiles:
        begin(g, here)

    def trip(i, carry):
        n = 2 * i
        lax.fori_loop(item(n)[3], item(jnp.minimum(n + 2, items - 1))[3], arrive, 0)

        @pl.when(i == lax.div(items, 4))
        def _():
            wo_a(0).wait_recv()
            if xa_hops > 1:
                wo_a(1).start()
            if xb_hops:
                wo_b(0).wait_recv()

        @pl.when(i == lax.div(items * 7, 16))
        def _():
            if xa_hops > 1:
                wo_a(1).wait_recv()
            for d in range(1, tp):
                wo_mate(d).start()

        for b in range(2):
            now = n + b
            scores = score_stage(jnp.minimum(now + 1, items - 1), 1 - b)
            sums_now = sum_stage(now, b)
            for g, h, here in tiles:
                scores(g, here)
                sums_now(g, here, h)
        return carry

    def to_mate(q):
        return remote(
            acc.at[2 * q + 1 - side], x_in.at[q], x_send.at[q], x_recv.at[q], "sp", mate
        )

    def merged(q):
        mine = 2 * q + side
        a_mass, a_peak = acc[mine, MASS:MASS + 1, :], peak[mine]
        b_mass, b_peak = x_in[q, MASS:MASS + 1, :], x_in[q, PEAK:PEAK + 1, :]
        top = jnp.maximum(a_peak, b_peak)
        wa, wb = jnp.exp(a_peak - top), jnp.exp(b_peak - top)
        return top, a_mass * wa + b_mass * wb, wa, wb

    def sums_of(q, wa, wb, here):
        return (
            acc[2 * q + side, AUG - CUT:, here] * wa[:, here] + x_in[q, AUG - CUT:, here] * wb[:, here]
        )

    ret_copies = [
        remote(ret_o, in_o, r_send.at[0], r_recv.at[0], "sp", partner),
        remote(ret_s, in_s, r_send.at[1], r_recv.at[1], "sp", partner),
    ]
    half_trips = lax.div(partner_items + 1, 2)
    lax.fori_loop(0, half_trips, trip, 0)

    @pl.when(jnp.logical_not(heavy))
    def _():
        acc[3 - side, PEAK:PEAK + 1, :] = peak[3 - side]
        to_mate(1).start()
        to_mate(1).wait_recv()
        top, mass, wa, wb = merged(1)
        inverse = 1.0 / mass
        for h in range(heads):
            here = slice(h * local_rows, (h + 1) * local_rows)
            ret_o[:, here] = (sums_of(1, wa, wb, here) * inverse[:, here]).astype(bf)
        ret_s[0:1, :] = top
        ret_s[1:2, :] = mass
        for copy in ret_copies:
            copy.start()

    lax.fori_loop(half_trips, lax.div(items, 2), trip, 0)
    acc[1 - side, PEAK:PEAK + 1, :] = peak[1 - side]
    to_mate(0).start()
    to_mate(0).wait_recv()
    top, mass, wa, wb = merged(0)

    @pl.when(jnp.logical_not(heavy))
    def _():
        inverse = 1.0 / mass
        for h in range(heads):
            here = slice(h * local_rows, (h + 1) * local_rows)
            att_t[h * HEAD:(h + 1) * HEAD, :] = (sums_of(0, wa, wb, here) * inverse[:, here]).astype(bf)

    @pl.when(heavy)
    def _():
        for copy in ret_copies:
            copy.wait_recv()
        r_top, r_mass = in_s[0:1, :], in_s[1:2, :]
        best = jnp.maximum(top, r_top)
        w_own, w_far = jnp.exp(top - best), jnp.exp(r_top - best) * r_mass
        inverse = 1.0 / (mass * w_own + w_far)
        w_own, w_far = w_own * inverse, w_far * inverse
        for h in range(heads):
            here = slice(h * local_rows, (h + 1) * local_rows)
            att_t[h * HEAD:(h + 1) * HEAD, :] = (
                sums_of(0, wa, wb, here) * w_own[:, here] + in_o[:, here].astype(f32) * w_far[:, here]
            ).astype(bf)

    att_out[...] = att_t[...].T.reshape(tp, rows, q_cols)

    def att_copy(d):
        to = lax.rem(x + d, tp)
        return remote(att_out.at[to], att_all.at[x], att_send.at[d - 1], att_recv.at[d - 1], "tp", to)

    for d in range(1, tp):
        att_copy(d).start()
    att_all[x] = att_out[x]
    for k in range(chunks):
        for d in range(xa_hops):
            tok_a(d, k).wait_send()
        for d in range(xb_hops):
            tok_b(d, k).wait_send()
    sum_copy.wait_send()
    q_copy.wait_send()

    def drain_total(d, carry):
        tell(d).wait_send()
        return carry

    lax.fori_loop(1, far_n, drain_total, 0)
    for d in range(xa_hops):
        wo_a(d).wait_send()
    for d in range(xb_hops):
        wo_b(d).wait_send()
    for d in range(1, nz):
        target, copy = column(d)

        @pl.when(needs(z, target))
        def _():
            copy.wait_send()

    def drain(e, carry):
        r, along_a, along_b = event(e)

        @pl.when(along_a)
        def _():
            ring_a(r).wait_send()

        @pl.when(along_b)
        def _():
            ring_b(r).wait_send()

        return carry

    lax.fori_loop(0, row_n * ny, drain, 0)
    to_mate(0).wait_send()

    @pl.when(heavy)
    def _():
        partner_q.wait_send()

    @pl.when(jnp.logical_not(heavy))
    def _():
        forward_q.wait_send()
        to_mate(1).wait_send()

    for d in range(1, tp):
        wo_mate(d).wait_recv()
    for d in range(1, tp):
        att_copy(d).wait_recv()
    for k in range(4):
        span = slice(k * (out_cols // 4), (k + 1) * (out_cols // 4))
        value = None
        for r in range(tp):
            term = jnp.dot(
                att_all[r], wo_all[r, :, :, span].reshape(q_cols, out_cols // 4),
                preferred_element_type=f32,
            ).astype(bf).astype(f32)
            value = term if value is None else value + term
        out[:, span] = value.astype(bf)

    for d in range(1, tp):
        wo_mate(d).wait_send()
        att_copy(d).wait_send()

    @pl.when(jnp.logical_not(heavy))
    def _():
        for copy in ret_copies:
            copy.wait_send()


def shards(ny, tokens, w_query, w_key, w_value, w_gate, gate_bias, w_output):
    sp = lax.axis_size("sp")
    tp = lax.axis_size("tp")
    rows, width = tokens.shape
    local_rows = rows * tp
    q_cols, key_cols, heads = w_query.shape[1], w_key.shape[1], w_gate.shape[1]
    out_cols = w_output.shape[1]
    assert key_cols == HEAD and heads == 4 and q_cols == heads * HEAD
    chunks = 8 if width % 1024 == 0 else 2
    far_n = sp // 2
    nz = far_n // ny
    lanes = heads * local_rows
    ka_rows = key_cols + AUG
    xa, xb = tp // 2, max(tp // 2 - 1, 1)
    dma = pltpu.SemaphoreType.DMA
    hbm_spec = pl.BlockSpec(memory_space=pltpu.HBM)
    vmem_spec = pl.BlockSpec(memory_space=pltpu.VMEM)
    operands = (tokens, w_query, w_key.T, w_value.T, w_gate.T, gate_bias, w_output)
    vmem = pltpu.VMEM
    return pl.pallas_call(
        functools.partial(kernel, sp, tp, ny, chunks),
        out_shape=jax.ShapeDtypeStruct((rows, out_cols), bf),
        in_specs=[hbm_spec] * 7,
        out_specs=vmem_spec,
        scratch_shapes=[
            vmem((tp, rows, width), bf),
            vmem((width, q_cols), bf),
            vmem((q_cols + 2 * key_cols + AUG, width), bf),
            vmem((heads, width), bf),
            vmem((tp, 2, q_cols // 2, out_cols), bf),
            vmem((q_cols + 2 * key_cols + AUG, local_rows), f32),
            vmem((far_n, ka_rows + key_cols, local_rows), bf),
            vmem((4, ka_rows, lanes), bf),
            vmem((far_n, 1, LANES), f32),
            vmem((far_n, 1, LANES), f32),
            vmem((far_n, heads * LANES), f32),
            vmem((far_n, heads * LANES), f32),
            vmem((2, 2, local_rows, lanes), f32),
            vmem((2, 2, 1, lanes), f32),
            vmem((4, 1, lanes), f32),
            vmem((4, ka_rows - CUT, lanes), f32),
            vmem((2, ka_rows - CUT, lanes), f32),
            vmem((key_cols, lanes), bf),
            vmem((8, lanes), f32),
            vmem((key_cols, lanes), bf),
            vmem((8, lanes), f32),
            vmem((q_cols, local_rows), bf),
            vmem((tp, rows, q_cols), bf),
            vmem((tp, rows, q_cols), bf),
            pltpu.SMEM((heads,), f32),
            dma((7,)),
            dma,
            dma((xa, chunks)),
            dma((xa, chunks)),
            dma((xb, chunks)),
            dma((xb, chunks)),
            dma,
            dma,
            dma((far_n,)),
            dma((far_n,)),
            dma,
            dma,
            dma,
            dma,
            dma,
            dma,
            dma((nz,)),
            dma((far_n,)),
            dma((far_n,)),
            dma((far_n,)),
            dma((xa,)),
            dma((xa,)),
            dma((xb,)),
            dma((xb,)),
            dma((tp - 1,)),
            dma((tp - 1,)),
            dma((2,)),
            dma((2,)),
            dma((2,)),
            dma((2,)),
            dma((tp - 1,)),
            dma((tp - 1,)),
        ],
        compiler_params=pltpu.CompilerParams(
            collective_id=0, has_side_effects=True, vmem_limit_bytes=60 << 20
        ),
    )(*(pltpu.with_memory_space_constraint(x, pltpu.HBM) for x in operands))


def solution(mesh):
    return jax.shard_map(
        functools.partial(shards, min(RING, mesh.shape["sp"] // 4)),
        mesh=mesh,
        in_specs=(
            P(("sp", "tp"), None),
            P(None, "tp"),
            P(None, "tp"),
            P(None, "tp"),
            P(None, "tp"),
            P("tp"),
            P("tp", None),
        ),
        out_specs=P(("sp", "tp"), None),
        check_vma=False,
    )
```

```python
import functools

import jax
import jax.numpy as jnp
from jax import lax
from jax.experimental import pallas as pl
from jax.experimental.pallas import tpu as pltpu
from jax.sharding import PartitionSpec as P

HEAD = 64
LANES = 128
AUG = 16
RING = 8
CUT = 8
MASS, PEAK = 12 - CUT, 13 - CUT
masked_value = -1e30
skipped_value = -1e38
MESH = pl.DeviceIdType.MESH
f32, bf = jnp.float32, jnp.bfloat16


def pieces_of(x):
    a = x.astype(bf)
    r = x - a.astype(f32)
    b = r.astype(bf)
    c = (r - b.astype(f32)).astype(bf)
    return a, b, c


LAG = 6


def plan(z, nz, ny):
    deep = nz // 2
    heavy = z >= deep
    kept = range(z - deep + 1, z + 1) if heavy else range(z + 1)
    lent = () if heavy else range(deep - z)
    others = sorted(set(kept) | set(lent), key=lambda row: (abs(row - z), row))[1:]
    own = [(z, step) for step in range(1, ny)]
    events = []
    queue = list(own[:-1]) if ny > 2 else list(own)
    for row in others:
        events += queue[:2] + [(row, 0)]
        queue = queue[2:]
    events += queue
    late = own[len(own) - 1:] if ny > 2 else []
    split = [(z - deep if heavy else deep - 1 - z, step) for step in range(min(3, ny - 1))]
    split = split if deep >= 3 else []
    shared = split if heavy else []
    for step in range(1, ny):
        events += [(row, step) for row in others]
        if step == 2:
            events += late
        if step == 1:
            events += shared[:1]
        if step == min(3, ny - 1):
            events += shared[1:]
    ahead = min(6, len(events))
    place = {event: at + 1 for at, event in enumerate(events)}
    place[(z, 0)] = 0
    first = [(event, 0) for event in own[:-1]]
    keep = [event for event in events if event[0] in kept and (event, 0) not in first]
    lend = ([(z, 0)] if z in lent else []) + [event for event in events if event[0] in lent]
    lend = [event for event in lend if event not in split]
    if heavy:
        items = [(event, 0) for event in events]
        fast = first[:4]
        items = fast + [item for item in items if item not in fast]
    else:
        items = first[:4]
        keep = sorted([event for event, _ in first[4:]] + keep, key=lambda event: place[event])
        waiting = list(keep)
        for at in range(len(events) + 1):
            items += [(event, 1) for event in lend if place[event] == at]
            while waiting and place[waiting[0]] <= at - LAG:
                items.append((waiting.pop(0), 0))
        items += [(event, 0) for event in waiting]
    lent_end = max([at + 1 for at, item in enumerate(items) if item[1] == 1], default=len(items))
    table, need = [], ahead
    for (row, step), q in items:
        need = max(need, place[(row, step)])
        table.append((row, step, q, 0, need))
    if len(table) % 2:
        table.append(table[-1][:2] + (0, 1, need))
    lent_end = len(table) if heavy else min((lent_end + 1) // 2 * 2, len(table))
    return events, ahead, table, lent_end


def kernel(
    sp, tp, ny, chunks,
    tokens, w_query, w_key, w_value, w_gate, bias_in, w_output,
    out,
    tok, wq_raw, wt, w_g, wo_all, proj, kx, qa, sums, pair_sums, gk, gq,
    score, tile_max, peak, acc, x_in, ret_o, ret_s, in_o, in_s,
    att_t, att_out, att_all, bias,
    local_sem, own_sem, ta_send, ta_recv, tb_send, tb_recv,
    sum_send, sum_recv, tot_send, tot_recv, onward_send,
    q_send, q_recv, pq_send, pq_recv, fq_send, fq_recv,
    z_send, a_send, b_send, kx_recv,
    wa_send, wa_recv, wb_send, wb_recv, wm_send, wm_recv,
    x_send, x_recv, r_send, r_recv, att_send, att_recv,
):
    me = lax.axis_index("sp")
    x = lax.axis_index("tp")
    far_n = sp // 2
    nz = far_n // ny
    deep = nz // 2
    far, side = lax.div(me, 2), lax.rem(me, 2)
    z, y = lax.div(far, ny), lax.rem(far, ny)
    mate = far * 2 + (1 - side)
    sign = 1 - 2 * side
    rows = tok.shape[1]
    local_rows = rows * tp
    width = tok.shape[2]
    q_cols = w_query.shape[1]
    heads = w_gate.shape[0]
    key_cols = w_key.shape[0]
    piece = width // chunks
    kv_at = q_cols
    gate_at = q_cols + 2 * key_cols
    ka_rows = key_cols + AUG
    lanes = heads * local_rows
    out_cols = w_output.shape[1]
    a_hops, b_hops = ny // 2, ny // 2 - 1
    xa_hops, xb_hops = tp // 2, tp // 2 - 1
    heavy = z >= deep
    other_z = nz - 1 - z
    partner_far = other_z * ny + y
    partner = partner_far * 2 + side
    x_a = lax.rem(x + sign + tp, tp)
    x_b = lax.rem(x - sign + tp, tp)
    y_a = (z * ny + lax.rem(y + sign + ny, ny)) * 2 + side
    y_b = (z * ny + lax.rem(y - sign + ny, ny)) * 2 + side

    loads = [
        pltpu.make_async_copy(w_query, wq_raw, local_sem.at[0]),
        pltpu.make_async_copy(w_key, wt.at[pl.ds(kv_at, key_cols)], local_sem.at[1]),
        pltpu.make_async_copy(w_value, wt.at[pl.ds(kv_at + key_cols, key_cols)], local_sem.at[2]),
        pltpu.make_async_copy(w_gate, w_g, local_sem.at[3]),
        pltpu.make_async_copy(bias_in, bias, local_sem.at[4]),
        pltpu.make_async_copy(w_output.at[pl.ds(0, q_cols // 2)], wo_all.at[x, 0], local_sem.at[5]),
        pltpu.make_async_copy(w_output.at[pl.ds(q_cols // 2, q_cols // 2)], wo_all.at[x, 1], local_sem.at[6]),
    ]
    own = pltpu.make_async_copy(tokens, tok.at[x], own_sem)
    own.start()
    for load in loads:
        load.start()

    barrier = pltpu.get_barrier_semaphore()
    for d in range(1, tp):
        pl.semaphore_signal(barrier, inc=1, device_id={"tp": lax.rem(x + d, tp)}, device_id_type=MESH)
    pl.semaphore_signal(barrier, inc=1, device_id={"sp": mate}, device_id_type=MESH)

    def greet(d, carry):
        other = lax.rem(far + d, far_n) * 2 + side
        pl.semaphore_signal(barrier, inc=1, device_id={"sp": other}, device_id_type=MESH)
        return carry

    lax.fori_loop(1, far_n, greet, 0)
    pl.semaphore_wait(barrier, (tp - 1) + 1 + (far_n - 1))

    def remote(src, dst, send, recv, axis, index):
        return pltpu.make_async_remote_copy(
            src, dst, send, recv, device_id={axis: index}, device_id_type=MESH
        )

    def tok_a(d, k):
        ref = tok.at[lax.rem(x - sign * d + tp, tp), :, pl.ds(k * piece, piece)]
        return remote(ref, ref, ta_send.at[d, k], ta_recv.at[d, k], "tp", x_a)

    def tok_b(d, k):
        ref = tok.at[lax.rem(x + sign * d + tp, tp), :, pl.ds(k * piece, piece)]
        return remote(ref, ref, tb_send.at[d, k], tb_recv.at[d, k], "tp", x_b)

    own.wait()
    for k in range(chunks):
        tok_a(0, k).start()
        if xb_hops:
            tok_b(0, k).start()

    for load in loads[:5]:
        load.wait()
    build = 256
    for i in range(width // build):
        wt[0:q_cols, i * build:(i + 1) * build] = wq_raw[i * build:(i + 1) * build, :].T
    wt[gate_at:gate_at + AUG, :] = jnp.concatenate(
        [w_g[...].astype(f32), jnp.zeros((AUG - heads, width), f32)], axis=0
    ).astype(bf)

    q_row = lax.broadcasted_iota(jnp.int32, (AUG, lanes), 0)
    q_head = lax.div(lax.broadcasted_iota(jnp.int32, (AUG, lanes), 1), local_rows)
    pattern = jnp.where(
        (q_row < 3 * heads) & (lax.rem(q_row, heads) == q_head), 1.0, 0.0
    ).astype(bf)
    for i in range(4):
        qa[i, key_cols:ka_rows, :] = pattern

    def relay(d, k):
        tok_a(d - 1, k).wait_recv()
        if d < xa_hops:
            tok_a(d, k).start()
        if d <= xb_hops:
            tok_b(d - 1, k).wait_recv()
            if d < xb_hops:
                tok_b(d, k).start()

    for d in range(1, xa_hops):
        for k in range(chunks):
            relay(d, k)
    for k in range(chunks):
        relay(xa_hops, k)
        here = tok[:, :, k * piece:(k + 1) * piece].reshape(local_rows, piece)
        part = lax.dot_general(
            wt[:, k * piece:(k + 1) * piece], here, (((1,), (1,)), ((), ())),
            preferred_element_type=f32,
        )
        if k == 0:
            proj[...] = part
        else:
            proj[...] += part

    row_of = lax.broadcasted_iota(jnp.int32, (8, local_rows), 0)
    u = proj[gate_at:gate_at + 8, :].astype(bf).astype(f32)
    for h in range(heads):
        u = jnp.where(row_of == h, u + bias[h], u)
    gates = jnp.minimum(u, 0.0) - jnp.log1p(jnp.exp(-jnp.abs(u)))
    gates = jnp.where(row_of < heads, gates, 0.0)
    upper = (
        lax.broadcasted_iota(jnp.int32, (local_rows, local_rows), 0)
        <= lax.broadcasted_iota(jnp.int32, (local_rows, local_rows), 1)
    )
    ones = jnp.where(upper, 1.0, 0.0).astype(bf)
    g0, g1, g2 = pieces_of(gates)
    total = jnp.dot(g2, ones, preferred_element_type=f32)
    total = total + jnp.dot(g1, ones, preferred_element_type=f32)
    total = total + jnp.dot(g0, ones, preferred_element_type=f32)
    pick = (
        lax.broadcasted_iota(jnp.int32, (8, LANES), 0)
        == lax.div(lax.broadcasted_iota(jnp.int32, (8, LANES), 1), LANES // heads)
    )
    block_sum = jnp.broadcast_to(total[:, local_rows - 1:], (8, LANES))
    sums[far] = jnp.sum(jnp.where(pick, block_sum, 0.0), axis=0, keepdims=True)

    def tell(d):
        return remote(
            sums.at[far], sums.at[far], tot_send.at[d], tot_recv.at[far],
            "sp", lax.rem(far + d, far_n) * 2 + side,
        )

    def hear(d):
        r = lax.rem(far + d, far_n)
        return remote(sums.at[r], sums.at[r], tot_send.at[d], tot_recv.at[r], "sp", r * 2 + side)

    def send_total(d, carry):
        tell(d).start()
        return carry

    lax.fori_loop(1, far_n, send_total, 0)

    s0, s1, s2 = [p.astype(f32)[:heads] for p in pieces_of(-total)]
    last = jnp.where(lax.broadcasted_iota(jnp.int32, (AUG - 3 * heads, local_rows), 0) == 0, 1.0, 0.0)
    kx[far, 0:key_cols, :] = proj[kv_at:kv_at + key_cols, :].astype(bf)
    kx[far, key_cols:ka_rows, :] = jnp.concatenate([s0, s1, s2, last], axis=0).astype(bf)
    kx[far, ka_rows:, :] = proj[kv_at + key_cols:kv_at + 2 * key_cols, :].astype(bf)

    def ring_a(r):
        return remote(kx.at[r], kx.at[r], a_send.at[r], kx_recv.at[r], "sp", y_a)

    def ring_b(r):
        return remote(kx.at[r], kx.at[r], b_send.at[r], kx_recv.at[r], "sp", y_b)

    def needs(row, at):
        low = jnp.where(at >= deep, at - deep + 1, 0)
        high = jnp.where(at >= deep, at, jnp.maximum(at, deep - 1 - at))
        return (row >= low) & (row <= high)

    def column(d):
        target = lax.rem(z + d, nz)
        return target, remote(
            kx.at[far], kx.at[far], z_send.at[d - 1], kx_recv.at[far],
            "sp", (target * ny + y) * 2 + side,
        )

    def direct(d, target):
        return jnp.logical_not((target >= deep) & (d == deep - 1) & (deep >= 3))

    def onward(r, way):
        return remote(
            kx.at[r], kx.at[r], onward_send.at[way], kx_recv.at[r], "sp",
            (lax.rem(z + 1, nz) * ny + y) * 2 + side,
        )

    ring_a(far).start()
    if b_hops:
        ring_b(far).start()
    for d in range(1, nz):
        target, copy = column(d)

        @pl.when(needs(z, target) & direct(d, target))
        def _():
            copy.start()

    scale = HEAD ** -0.5
    for h in range(heads):
        qa[side, 0:key_cols, h * local_rows:(h + 1) * local_rows] = (
            proj[h * HEAD:(h + 1) * HEAD, :].astype(bf) * bf(scale)
        )

    q_half = pl.ds(0, key_cols)
    q_copy = remote(qa.at[side, q_half], qa.at[side, q_half], q_send, q_recv, "sp", mate)
    q_copy.start()
    partner_q = remote(qa.at[side, q_half], qa.at[2 + side, q_half], pq_send, pq_recv, "sp", partner)
    forward_q = remote(qa.at[2 + side, q_half], qa.at[2 + side, q_half], fq_send, fq_recv, "sp", mate)

    @pl.when(heavy)
    def _():
        partner_q.start()

    for load in loads[5:]:
        load.wait()

    def wo_a(d):
        ref = wo_all.at[lax.rem(x - sign * d + tp, tp), side]
        return remote(ref, ref, wa_send.at[d], wa_recv.at[d], "tp", x_a)

    def wo_b(d):
        ref = wo_all.at[lax.rem(x + sign * d + tp, tp), side]
        return remote(ref, ref, wb_send.at[d], wb_recv.at[d], "tp", x_b)

    def wo_mate(d):
        ref = wo_all.at[lax.rem(x + d, tp), side]
        return remote(ref, ref, wm_send.at[d - 1], wm_recv.at[d - 1], "sp", mate)

    wo_a(0).start()
    if xb_hops:
        wo_b(0).start()

    def doubled(row, h):
        part = row[:, h * LANES:(h + 1) * LANES]
        return jnp.concatenate([part] * (local_rows // LANES), axis=1)

    q_copy.wait_recv()
    key_at = lax.broadcasted_iota(jnp.int32, (local_rows, local_rows), 0) + side * local_rows
    query_at = lax.broadcasted_iota(jnp.int32, (local_rows, local_rows), 1)
    ka = kx[far, 0:ka_rows, :].T
    va = kx[far, key_cols:, :]
    for g in range(2):
        allowed = key_at <= query_at + g * local_rows
        for h in range(heads):
            here = slice(h * local_rows, (h + 1) * local_rows)
            s = jnp.dot(ka, qa[g, :, here], preferred_element_type=f32)
            s = jnp.where(allowed, s, masked_value)
            top = jnp.max(s, axis=0, keepdims=True)
            peak[g, :, here] = top
            term = jnp.dot(va, jnp.exp(s - top).astype(bf), preferred_element_type=f32)
            acc[g, :, here] = term[CUT:]
    peak[2:4] = jnp.full((2, 1, lanes), masked_value, f32)
    acc[2:4] = jnp.zeros((2,) + acc.shape[1:], f32)

    kinds = []
    for at in list(range(deep)) + [deep]:
        event_list, first_events, item_list, lent_end = plan(at, nz, ny)
        event_codes, item_codes = [], []
        for row, step in event_list:
            d = (step + 1) // 2
            spread = step == 0 or not (at >= deep and at - row == deep)
            along = int((step == 0 or step % 2 == 1) and d < a_hops and spread)
            back = int(step % 2 == 0 and d < b_hops and spread)
            event_codes.append(((at - row + nz) * 16 + step) * 4 + along * 2 + back)
        for row, step, q, pad, need in item_list:
            item_codes.append((((at - row + nz) * 16 + step) * 4 + q * 2 + pad) * 64 + need)
        kinds.append((event_codes, item_codes, first_events, lent_end))

    def by_kind(values):
        chosen = jnp.int32(values[deep])
        for at in range(deep):
            if values[at] != values[deep]:
                chosen = jnp.where(z == at, values[at], chosen)
        return chosen

    def column_of(index):
        size = max(len(kind[index]) for kind in kinds)
        return [by_kind([(kind[index] + [0] * size)[n] for kind in kinds]) for n in range(size)]

    all_events, all_items = column_of(0), column_of(1)
    events = by_kind([len(kind[0]) for kind in kinds])
    items = by_kind([len(kind[1]) for kind in kinds])
    ahead = by_kind([kind[2] for kind in kinds])
    partner_items = by_kind([kind[3] for kind in kinds])

    def lookup(codes, n):
        level, codes = 1, list(codes)
        while len(codes) > 1:
            odd = lax.rem(lax.div(n, level), 2) == 1
            codes = [
                jnp.where(odd, codes[k + 1], codes[k]) if k + 1 < len(codes) else codes[k]
                for k in range(0, len(codes), 2)
            ]
            level *= 2
        return codes[0]

    def tile_of(place):
        away, step = lax.div(place, 16) - nz, lax.rem(place, 16)
        d, odd = lax.div(step + 1, 2), lax.rem(step, 2)
        source = lax.rem(y + jnp.where(odd == 1, -d, d) * sign + ny, ny)
        return (z - away) * ny + source, away, step

    def event(e):
        code = lookup(all_events, e)
        r, away, step = tile_of(lax.div(code, 4))
        ways = lax.rem(code, 4)
        pass_on = (step == 0) & (z + 1 >= deep) & (z + 1 < nz) & (deep >= 3)
        along_z = jnp.where(
            pass_on & (away == deep - 2), 1, jnp.where(pass_on & (away == deep - 1), 2, 0)
        )
        return r, ways >= 2, lax.rem(ways, 2) == 1, along_z

    def arrive(e, carry):
        r, along_a, along_b, along_z = event(e)
        ring_a(r).wait_recv()

        for way in range(2):
            @pl.when(along_z == way + 1)
            def _():
                onward(r, way).start()

        @pl.when(along_a)
        def _():
            ring_a(r).start()

        @pl.when(along_b)
        def _():
            ring_b(r).start()

        return carry

    lax.fori_loop(0, ahead, arrive, 0)

    def hear_total(d, carry):
        hear(d).wait_recv()
        return carry

    lax.fori_loop(1, far_n, hear_total, 0)
    sum_copy = remote(sums, pair_sums, sum_send, sum_recv, "sp", mate)
    sum_copy.start()
    lower = (
        lax.broadcasted_iota(jnp.int32, (far_n, far_n), 1)
        < lax.broadcasted_iota(jnp.int32, (far_n, far_n), 0)
    )
    below = jnp.where(lower, 1.0, 0.0).astype(bf)
    sum_copy.wait_recv()
    pair_table = pair_sums[...].reshape(far_n, LANES)
    start_table = jnp.where(side == 1, pair_table, 0.0)
    t0, t1, t2 = pieces_of(sums[...].reshape(far_n, LANES) + pair_table)
    before = jnp.dot(below, t2, preferred_element_type=f32)
    before = before + jnp.dot(below, t1, preferred_element_type=f32)
    before = before + jnp.dot(below, t0, preferred_element_type=f32)
    starts = before + start_table
    for h in range(heads):
        at = h * (LANES // heads)
        span = slice(h * LANES, (h + 1) * LANES)
        gq[:, span] = jnp.broadcast_to(before[:, at:at + 1], (far_n, LANES))
        gk[:, span] = jnp.broadcast_to(starts[:, at:at + 1], (far_n, LANES))

    own_shift = gq[pl.ds(far, 1), :] - gk[pl.ds(far, 1), :]
    for g in range(2):
        for h in range(heads):
            here = slice(h * local_rows, (h + 1) * local_rows)
            peak[g, :, here] = peak[g, :, here] + doubled(own_shift, h)

    def item(n):
        code = lookup(all_items, n)
        head = lax.div(code, 64)
        r, away, _ = tile_of(lax.div(head, 4))
        q = lax.div(lax.rem(head, 4), 2)
        skip = (lax.rem(head, 2) == 1) | ((q == 0) & (away == 0) & (r > far))
        return r, q, jnp.where(skip, 1, 0), lax.rem(code, 64)

    def score_stage(chosen, b):
        r, q, _, _ = chosen
        ka = kx[r, 0:ka_rows, :].T

        def run(g, here):
            s = jnp.dot(ka, qa[2 * q + g, :, here], preferred_element_type=f32)
            score[b, g, :, here] = s
            tile_max[b, g, :, here] = jnp.max(s, axis=0, keepdims=True)

        return run

    def sum_stage(chosen, b):
        r, q, skip, _ = chosen
        va = kx[r, key_cols:, :]
        chip = jnp.where(q == 0, far, partner_far)
        offset = gq[pl.ds(chip, 1), :] - gk[pl.ds(r, 1), :]
        offset = jnp.where(skip == 1, skipped_value, offset)

        def run(g, here, h):
            o = doubled(offset, h)
            old = peak[2 * q + g, :, here]
            new = jnp.maximum(old, tile_max[b, g, :, here] + o)
            weight = jnp.exp(score[b, g, :, here] - (new - o)).astype(bf)
            rescale = jnp.exp(old - new)
            peak[2 * q + g, :, here] = new
            term = jnp.dot(va, weight, preferred_element_type=f32)
            acc[2 * q + g, :, here] = acc[2 * q + g, :, here] * rescale + term[CUT:]

        return run

    tiles = [(g, h, slice(h * local_rows, (h + 1) * local_rows)) for g in range(2) for h in range(heads)]

    def take_partner_q():
        partner_q.wait_recv()
        forward_q.start()
        forward_q.wait_recv()

    if ny < 8:
        pl.when(jnp.logical_not(heavy))(take_partner_q)
    opening = item(jnp.int32(0))
    lax.fori_loop(ahead, opening[3], arrive, 0)
    begin = score_stage(opening, 0)
    for g, h, here in tiles:
        begin(g, here)

    def trip(i, carry):
        n = 2 * i
        if ny >= 8:
            pl.when(jnp.logical_not(heavy) & (i == 1))(take_partner_q)
        chosen = carry
        lax.fori_loop(chosen[0][3], chosen[2][3], arrive, 0)

        @pl.when(i == lax.div(items, 4))
        def _():
            wo_a(0).wait_recv()
            if xa_hops > 1:
                wo_a(1).start()
            if xb_hops:
                wo_b(0).wait_recv()

        @pl.when(i == lax.div(items * 7, 16))
        def _():
            if xa_hops > 1:
                wo_a(1).wait_recv()
            for d in range(1, tp):
                wo_mate(d).start()

        for b in range(2):
            scores = score_stage(chosen[b + 1], 1 - b)
            sums_now = sum_stage(chosen[b], b)
            for g, h, here in tiles:
                scores(g, here)
                sums_now(g, here, h)
        return (chosen[2],) + tuple(item(jnp.minimum(n + k, items - 1)) for k in (3, 4))

    def to_mate(q):
        return remote(
            acc.at[2 * q + 1 - side], x_in.at[q], x_send.at[q], x_recv.at[q], "sp", mate
        )

    def merged(q):
        mine = 2 * q + side
        a_mass, a_peak = acc[mine, MASS:MASS + 1, :], peak[mine]
        b_mass, b_peak = x_in[q, MASS:MASS + 1, :], x_in[q, PEAK:PEAK + 1, :]
        top = jnp.maximum(a_peak, b_peak)
        wa, wb = jnp.exp(a_peak - top), jnp.exp(b_peak - top)
        return top, a_mass * wa + b_mass * wb, wa, wb

    def sums_of(q, wa, wb, here):
        return (
            acc[2 * q + side, AUG - CUT:, here] * wa[:, here] + x_in[q, AUG - CUT:, here] * wb[:, here]
        )

    ret_copies = [
        remote(ret_o, in_o, r_send.at[0], r_recv.at[0], "sp", partner),
        remote(ret_s, in_s, r_send.at[1], r_recv.at[1], "sp", partner),
    ]
    half_trips = lax.div(partner_items + 1, 2)
    carried = (opening,) + tuple(item(jnp.minimum(jnp.int32(k), items - 1)) for k in (1, 2))
    carried = lax.fori_loop(0, half_trips, trip, carried)

    @pl.when(jnp.logical_not(heavy))
    def _():
        acc[3 - side, PEAK:PEAK + 1, :] = peak[3 - side]
        to_mate(1).start()
        to_mate(1).wait_recv()
        top, mass, wa, wb = merged(1)
        inverse = 1.0 / mass
        for h in range(heads):
            here = slice(h * local_rows, (h + 1) * local_rows)
            ret_o[:, here] = (sums_of(1, wa, wb, here) * inverse[:, here]).astype(bf)
        ret_s[0:1, :] = top
        ret_s[1:2, :] = mass
        for copy in ret_copies:
            copy.start()

    lax.fori_loop(half_trips, lax.div(items, 2), trip, carried)
    acc[1 - side, PEAK:PEAK + 1, :] = peak[1 - side]
    to_mate(0).start()
    to_mate(0).wait_recv()
    top, mass, wa, wb = merged(0)

    @pl.when(jnp.logical_not(heavy))
    def _():
        inverse = 1.0 / mass
        for h in range(heads):
            here = slice(h * local_rows, (h + 1) * local_rows)
            att_t[h * HEAD:(h + 1) * HEAD, :] = (sums_of(0, wa, wb, here) * inverse[:, here]).astype(bf)

    @pl.when(heavy)
    def _():
        for copy in ret_copies:
            copy.wait_recv()
        r_top, r_mass = in_s[0:1, :], in_s[1:2, :]
        best = jnp.maximum(top, r_top)
        w_own, w_far = jnp.exp(top - best), jnp.exp(r_top - best) * r_mass
        inverse = 1.0 / (mass * w_own + w_far)
        w_own, w_far = w_own * inverse, w_far * inverse
        for h in range(heads):
            here = slice(h * local_rows, (h + 1) * local_rows)
            att_t[h * HEAD:(h + 1) * HEAD, :] = (
                sums_of(0, wa, wb, here) * w_own[:, here] + in_o[:, here].astype(f32) * w_far[:, here]
            ).astype(bf)

    att_out[...] = att_t[...].T.reshape(tp, rows, q_cols)

    def att_copy(d):
        to = lax.rem(x + d, tp)
        return remote(att_out.at[to], att_all.at[x], att_send.at[d - 1], att_recv.at[d - 1], "tp", to)

    for d in range(1, tp):
        att_copy(d).start()
    att_all[x] = att_out[x]
    for k in range(chunks):
        for d in range(xa_hops):
            tok_a(d, k).wait_send()
        for d in range(xb_hops):
            tok_b(d, k).wait_send()
    sum_copy.wait_send()
    q_copy.wait_send()

    def drain_total(d, carry):
        tell(d).wait_send()
        return carry

    lax.fori_loop(1, far_n, drain_total, 0)
    for d in range(xa_hops):
        wo_a(d).wait_send()
    for d in range(xb_hops):
        wo_b(d).wait_send()
    for d in range(1, nz):
        target, copy = column(d)

        @pl.when(needs(z, target) & direct(d, target))
        def _():
            copy.wait_send()

    def drain(e, carry):
        r, along_a, along_b, along_z = event(e)

        for way in range(2):
            @pl.when(along_z == way + 1)
            def _():
                onward(r, way).wait_send()

        @pl.when(along_a)
        def _():
            ring_a(r).wait_send()

        @pl.when(along_b)
        def _():
            ring_b(r).wait_send()

        return carry

    ring_a(far).wait_send()
    if b_hops:
        ring_b(far).wait_send()
    lax.fori_loop(0, events, drain, 0)
    to_mate(0).wait_send()

    @pl.when(heavy)
    def _():
        partner_q.wait_send()

    @pl.when(jnp.logical_not(heavy))
    def _():
        forward_q.wait_send()
        to_mate(1).wait_send()

    for d in range(1, tp):
        wo_mate(d).wait_recv()
    for d in range(1, tp):
        att_copy(d).wait_recv()
    for k in range(4):
        span = slice(k * (out_cols // 4), (k + 1) * (out_cols // 4))
        value = None
        for r in range(tp):
            term = jnp.dot(
                att_all[r], wo_all[r, :, :, span].reshape(q_cols, out_cols // 4),
                preferred_element_type=f32,
            ).astype(bf).astype(f32)
            value = term if value is None else value + term
        out[:, span] = value.astype(bf)

    for d in range(1, tp):
        wo_mate(d).wait_send()
        att_copy(d).wait_send()

    @pl.when(jnp.logical_not(heavy))
    def _():
        for copy in ret_copies:
            copy.wait_send()


def shards(ny, tokens, w_query, w_key, w_value, w_gate, gate_bias, w_output):
    sp = lax.axis_size("sp")
    tp = lax.axis_size("tp")
    rows, width = tokens.shape
    local_rows = rows * tp
    q_cols, key_cols, heads = w_query.shape[1], w_key.shape[1], w_gate.shape[1]
    out_cols = w_output.shape[1]
    assert key_cols == HEAD and heads == 4 and q_cols == heads * HEAD
    chunks = 8 if width % 1024 == 0 else 2
    far_n = sp // 2
    nz = far_n // ny
    lanes = heads * local_rows
    ka_rows = key_cols + AUG
    xa, xb = tp // 2, max(tp // 2 - 1, 1)
    dma = pltpu.SemaphoreType.DMA
    hbm_spec = pl.BlockSpec(memory_space=pltpu.HBM)
    vmem_spec = pl.BlockSpec(memory_space=pltpu.VMEM)
    operands = (tokens, w_query, w_key.T, w_value.T, w_gate.T, gate_bias, w_output)
    vmem = pltpu.VMEM
    return pl.pallas_call(
        functools.partial(kernel, sp, tp, ny, chunks),
        out_shape=jax.ShapeDtypeStruct((rows, out_cols), bf),
        in_specs=[hbm_spec] * 7,
        out_specs=vmem_spec,
        scratch_shapes=[
            vmem((tp, rows, width), bf),
            vmem((width, q_cols), bf),
            vmem((q_cols + 2 * key_cols + AUG, width), bf),
            vmem((heads, width), bf),
            vmem((tp, 2, q_cols // 2, out_cols), bf),
            vmem((q_cols + 2 * key_cols + AUG, local_rows), f32),
            vmem((far_n, ka_rows + key_cols, local_rows), bf),
            vmem((4, ka_rows, lanes), bf),
            vmem((far_n, 1, LANES), f32),
            vmem((far_n, 1, LANES), f32),
            vmem((far_n, heads * LANES), f32),
            vmem((far_n, heads * LANES), f32),
            vmem((2, 2, local_rows, lanes), f32),
            vmem((2, 2, 1, lanes), f32),
            vmem((4, 1, lanes), f32),
            vmem((4, ka_rows - CUT, lanes), f32),
            vmem((2, ka_rows - CUT, lanes), f32),
            vmem((key_cols, lanes), bf),
            vmem((8, lanes), f32),
            vmem((key_cols, lanes), bf),
            vmem((8, lanes), f32),
            vmem((q_cols, local_rows), bf),
            vmem((tp, rows, q_cols), bf),
            vmem((tp, rows, q_cols), bf),
            pltpu.SMEM((heads,), f32),
            dma((7,)),
            dma,
            dma((xa, chunks)),
            dma((xa, chunks)),
            dma((xb, chunks)),
            dma((xb, chunks)),
            dma,
            dma,
            dma((far_n,)),
            dma((far_n,)),
            dma((2,)),
            dma,
            dma,
            dma,
            dma,
            dma,
            dma,
            dma((nz,)),
            dma((far_n,)),
            dma((far_n,)),
            dma((far_n,)),
            dma((xa,)),
            dma((xa,)),
            dma((xb,)),
            dma((xb,)),
            dma((tp - 1,)),
            dma((tp - 1,)),
            dma((2,)),
            dma((2,)),
            dma((2,)),
            dma((2,)),
            dma((tp - 1,)),
            dma((tp - 1,)),
        ],
        compiler_params=pltpu.CompilerParams(
            collective_id=0, has_side_effects=True, vmem_limit_bytes=60 << 20
        ),
    )(*(pltpu.with_memory_space_constraint(x, pltpu.HBM) for x in operands))


def solution(mesh):
    return jax.shard_map(
        functools.partial(shards, min(RING, mesh.shape["sp"] // 4)),
        mesh=mesh,
        in_specs=(
            P(("sp", "tp"), None),
            P(None, "tp"),
            P(None, "tp"),
            P(None, "tp"),
            P(None, "tp"),
            P("tp"),
            P("tp", None),
        ),
        out_specs=P(("sp", "tp"), None),
        check_vma=False,
    )
```
